32 devices in a mesh: rep: 2 (over x), fs: 8 (over z, y), tp: 2 (over core).
Axes of the slice: x: 2, y: 2, z: 4, core: 2. Of those that a mesh axis runs over, the one named last changes fastest.
Arguments:
- stream: bfloat16 [6144, 2048], P(('rep', 'fs'), 'tp'), may hold values from -24 to 24
- recurrence_input_weight: bfloat16 [2048, 2048], P('fs', 'tp'), may hold values from -0.125 to 0.125
- output_gate_weight: bfloat16 [2048, 2048], P('fs', 'tp'), may hold values from -0.125 to 0.125
- recurrence_gate_matrix: bfloat16 [16, 128, 128], P('tp'), may hold values from -0.5 to 0.5
- input_gate_matrix: bfloat16 [16, 128, 128], P('tp'), may hold values from -0.5 to 0.5
- channel_decay_rate: float32 [2048], P('tp')
- recurrence_taps: float32 [4, 2048], P(None, 'tp'), may hold values from -3 to 3
- spike_log_decay: float32 [6144, 16], P(('rep', 'fs'), 'tp'), may hold values from -2.1 to 0
- recurrence_output_weight: bfloat16 [2048, 2048], P('tp', 'fs'), may hold values from -0.3125 to 0.3125
- feedforward_gate_upward: bfloat16 [2048, 4096], P('fs', 'tp'), may hold values from -0.125 to 0.125
- feedforward_value_upward: bfloat16 [2048, 4096], P('fs', 'tp'), may hold values from -0.125 to 0.125
- feedforward_gate_taps: float32 [3, 4096], P(None, 'tp'), may hold values from -3 to 3
- feedforward_value_taps: float32 [3, 4096], P(None, 'tp'), may hold values from -3 to 3
- feedforward_down_weight: bfloat16 [4096, 2048], P('tp', 'fs'), may hold values from -0.1875 to 0.1875
- recurrence_norm_gain: float32 [2048], replicated, may hold values from 0.1 to 1.9
- feedforward_norm_gain: float32 [2048], replicated, may hold values from 0.1 to 1.9
- closing_norm_gain: float32 [2048], replicated, may hold values from 0.1 to 1.9
Outputs:
- layer_out: bfloat16 [6144, 2048], P(('rep', 'fs'), 'tp')
The draws below stay inside these ranges and needn't reach their ends.
All inputs are finite; a program needn't handle non-finite values.
Results may differ from the reference program's by a relative error of at most 0.018.
Values may be sent and summed in bfloat16 or wider, within the bound.
A program may use at most 64 MiB of HBM per device.

```python
import math
import jax
import jax.numpy as jnp
from jax import lax

MODEL_WIDTH = 2048
GATE_BLOCKS = 16
BLOCK = 128
R = 2048
FF = 4096
CONV = 4
FCONV = 3
SEQUENCE_TOKENS = 384
TOKEN_TOTAL = 6144
N_TP = 2


def draw_stream(key, part):
    row_key, sample_key = jax.random.split(jax.random.fold_in(key, 11), 2)
    samples = jax.random.truncated_normal(sample_key, -4.0, 4.0, (TOKEN_TOTAL, MODEL_WIDTH), jnp.float32)
    column_scale = jnp.exp(math.log(3.0) * jnp.arange(MODEL_WIDTH, dtype=jnp.float32) / MODEL_WIDTH)
    row_scale = jnp.exp(jax.random.uniform(row_key, (TOKEN_TOTAL, 1), jnp.float32, math.log(0.5), math.log(2.0)))
    return (samples * row_scale * column_scale[None, :]).astype(jnp.bfloat16)


def draw_channel_decay_rate(key, part):
    order_key, slow_key, fast_key = jax.random.split(jax.random.fold_in(key, 23), 3)
    ranking = jax.random.permutation(order_key, GATE_BLOCKS)
    slow_heads = ranking < GATE_BLOCKS // 2
    slow_rate = jnp.exp(jax.random.uniform(slow_key, (R,), jnp.float32, math.log(0.05), math.log(0.25))) / SEQUENCE_TOKENS
    fast_rate = jnp.exp(jax.random.uniform(fast_key, (R,), jnp.float32, math.log(0.006), math.log(0.025)))
    slow_mask = jnp.repeat(slow_heads, BLOCK)
    rate_per_step = jnp.where(slow_mask, slow_rate, fast_rate)
    return -jnp.log(jnp.expm1(rate_per_step))


def draw_spike_log_decay(key, part):
    position_random_key, depth_random_key = jax.random.split(jax.random.fold_in(key, 37), 2)
    sequence_count = TOKEN_TOTAL // SEQUENCE_TOKENS
    spike_positions = jax.random.randint(position_random_key, (sequence_count, 3, GATE_BLOCKS), 0, SEQUENCE_TOKENS)
    lower_limit = 0.5
    upper_limit = 0.8
    spike_depth = jnp.log(jax.random.uniform(depth_random_key, (sequence_count, 3, GATE_BLOCKS), jnp.float32, lower_limit, upper_limit))
    token_positions = jnp.arange(SEQUENCE_TOKENS)
    spike_hits = token_positions[None, None, :, None] == spike_positions[:, :, None, :]
    spike_total = jnp.sum(jnp.where(spike_hits, spike_depth[:, :, None, :], 0.0), axis=1)
    return spike_total.reshape(TOKEN_TOTAL, GATE_BLOCKS).astype(jnp.float32)


def steps_of(key, dims, shards, smallest, largest):
    factor_of = 1.0
    for dim, shards_of in shards:
        draws = jax.random.uniform(jax.random.fold_in(jax.random.fold_in(key, 6), dim), (shards_of,), jnp.float32, smallest / len(shards), largest / len(shards))
        factor_of = factor_of * jnp.repeat(jnp.exp(draws), dims[dim] // shards_of).reshape((-1,) + (1,) * (len(dims) - 1 - dim))
    return factor_of


def scatter_about(own_key, shape, spread, limit, shards=(), kind=jnp.bfloat16):
    result = jax.random.normal(own_key, shape, jnp.float32) * spread
    if len(shards) > 0:
        result = steps_of(own_key, shape, shards, -0.22, 0.18) * result
    return jnp.clip(result, min=-limit, max=limit).astype(kind)


def setup_inputs(seed: int = 0) -> dict:
    streams_of = jax.random.split(jax.random.key(seed), 18)
    stream = draw_stream(jax.random.fold_in(streams_of[17], 71), 0)
    recurrence_input_weight = scatter_about(streams_of[1], (MODEL_WIDTH, R), MODEL_WIDTH ** -0.5, 0.125, ((0, 8), (1, 2)))
    output_gate_weight = scatter_about(streams_of[2], (MODEL_WIDTH, R), MODEL_WIDTH ** -0.5, 0.125, ((0, 8), (1, 2)))
    recurrence_gate_matrix = scatter_about(streams_of[3], (GATE_BLOCKS, BLOCK, BLOCK), BLOCK ** -0.5, 0.5, ((0, 2),))
    input_gate_matrix = scatter_about(streams_of[4], (GATE_BLOCKS, BLOCK, BLOCK), BLOCK ** -0.5, 0.5, ((0, 2),))
    channel_decay_rate = draw_channel_decay_rate(jax.random.fold_in(streams_of[17], 71), 0)
    recurrence_taps = scatter_about(streams_of[6], (CONV, R), 0.5, 3.0, ((1, 2),), jnp.float32)
    spike_log_decay = draw_spike_log_decay(jax.random.fold_in(streams_of[17], 71), 0)
    recurrence_output_weight = scatter_about(streams_of[8], (R, MODEL_WIDTH), (R // 6) ** -0.5, 0.3125, ((0, 2), (1, 8)))
    feedforward_gate_upward = scatter_about(streams_of[9], (MODEL_WIDTH, FF), MODEL_WIDTH ** -0.5, 0.125, ((0, 8), (1, 2)))
    feedforward_value_upward = scatter_about(streams_of[10], (MODEL_WIDTH, FF), MODEL_WIDTH ** -0.5, 0.125, ((0, 8), (1, 2)))
    feedforward_gate_taps = scatter_about(streams_of[11], (FCONV, FF), 0.577, 3.0, ((1, 2),), jnp.float32)
    feedforward_value_taps = scatter_about(streams_of[12], (FCONV, FF), 0.577, 3.0, ((1, 2),), jnp.float32)
    feedforward_down_weight = scatter_about(streams_of[13], (FF, MODEL_WIDTH), (FF // 4) ** -0.5, 0.1875, ((0, 2), (1, 8)))
    recurrence_norm_gain = jnp.clip(1.0 + 0.18 * jax.random.normal(streams_of[14], (MODEL_WIDTH,), jnp.float32), 0.1, 1.9)
    feedforward_norm_gain = jnp.clip(1.0 + 0.18 * jax.random.normal(streams_of[15], (MODEL_WIDTH,), jnp.float32), 0.1, 1.9)
    closing_norm_gain = jnp.clip(1.0 + 0.18 * jax.random.normal(streams_of[16], (MODEL_WIDTH,), jnp.float32), 0.1, 1.9)
    return dict(stream=stream, recurrence_input_weight=recurrence_input_weight, output_gate_weight=output_gate_weight, recurrence_gate_matrix=recurrence_gate_matrix, input_gate_matrix=input_gate_matrix, channel_decay_rate=channel_decay_rate, recurrence_taps=recurrence_taps, spike_log_decay=spike_log_decay, recurrence_output_weight=recurrence_output_weight, feedforward_gate_upward=feedforward_gate_upward, feedforward_value_upward=feedforward_value_upward, feedforward_gate_taps=feedforward_gate_taps, feedforward_value_taps=feedforward_value_taps, feedforward_down_weight=feedforward_down_weight, recurrence_norm_gain=recurrence_norm_gain, feedforward_norm_gain=feedforward_norm_gain, closing_norm_gain=closing_norm_gain)


EPS = 1e-06
GATE_POWER = 8.0

def rms_scale(row_block, gain_vec):
    widened = row_block.astype(jnp.float32)
    inverse = lax.rsqrt(lax.optimization_barrier(jnp.mean(widened * widened, axis=-1, keepdims=True)) + EPS)
    return (widened * inverse * gain_vec).astype(jnp.bfloat16)

def causal_mix(values, kernel_taps):
    extent = kernel_taps.shape[0]
    length = values.shape[0]
    padded = jnp.pad(values, ((extent - 1, 0), (0, 0)))
    summed = kernel_taps[0] * padded[0:length]
    for offset in range(1, extent):
        summed = summed + kernel_taps[offset] * padded[offset:offset + length]
    return summed

def chain_step(earlier, following):
    return (earlier[0] * following[0], following[0] * earlier[1] + following[1])

def split_partials(left_rows, weight_rows, part_count):
    share_rows = left_rows.shape[1] // part_count
    summed = jnp.zeros((left_rows.shape[0], weight_rows.shape[1]), jnp.float32)
    for part_index in range(part_count):
        lower = part_index * share_rows
        partial_sum = jnp.dot(left_rows[:, lower:lower + share_rows], weight_rows[lower:lower + share_rows], preferred_element_type=jnp.float32).astype(jnp.bfloat16)
        summed = summed + lax.optimization_barrier(partial_sum).astype(jnp.float32)
    return summed

def reference(stream, recurrence_input_weight, output_gate_weight, recurrence_gate_matrix, input_gate_matrix, channel_decay_rate, recurrence_taps, spike_log_decay, recurrence_output_weight, feedforward_gate_upward, feedforward_value_upward, feedforward_gate_taps, feedforward_value_taps, feedforward_down_weight, recurrence_norm_gain, feedforward_norm_gain, closing_norm_gain):
    sequence_count = stream.shape[0] // SEQUENCE_TOKENS
    decay_base = (GATE_POWER * jax.nn.softplus(-channel_decay_rate)).reshape(GATE_BLOCKS, BLOCK)

    def single_sequence(input_rows):
        incoming_tokens, spike_events = input_rows
        normed = rms_scale(incoming_tokens, recurrence_norm_gain)
        rec_in = jnp.dot(normed, recurrence_input_weight, preferred_element_type=jnp.float32).astype(jnp.bfloat16)
        gate_src = jnp.dot(normed, output_gate_weight, preferred_element_type=jnp.float32).astype(jnp.bfloat16)
        conv_out = causal_mix(rec_in.astype(jnp.float32), recurrence_taps).astype(jnp.bfloat16)
        blocks = conv_out.astype(jnp.float32).reshape(SEQUENCE_TOKENS, GATE_BLOCKS, BLOCK)
        gate_restart = jax.nn.sigmoid(jnp.einsum('thi,hij->thj', blocks, recurrence_gate_matrix.astype(jnp.float32)))
        admit_gate = jax.nn.sigmoid(jnp.einsum('thi,hij->thj', blocks, input_gate_matrix.astype(jnp.float32)))
        decay_logarithm = -gate_restart * decay_base + spike_events[:, :, None]
        decay_rate = jnp.exp(decay_logarithm)
        inflow = jnp.sqrt(-jnp.expm1(2.0 * decay_logarithm)) * admit_gate * blocks
        states = lax.associative_scan(chain_step, (decay_rate, inflow), axis=0)[1]
        mixed_out = (states.reshape(SEQUENCE_TOKENS, R) * jax.nn.gelu(gate_src.astype(jnp.float32))).astype(jnp.bfloat16)
        branch = split_partials(mixed_out, recurrence_output_weight, N_TP).astype(jnp.bfloat16)
        middle = (incoming_tokens.astype(jnp.float32) + branch.astype(jnp.float32)).astype(jnp.bfloat16)
        normed_ffn = rms_scale(middle, feedforward_norm_gain)
        gate_up = jnp.dot(normed_ffn, feedforward_gate_upward, preferred_element_type=jnp.float32).astype(jnp.bfloat16)
        value_up = jnp.dot(normed_ffn, feedforward_value_upward, preferred_element_type=jnp.float32).astype(jnp.bfloat16)
        gate_conv = causal_mix(gate_up.astype(jnp.float32), feedforward_gate_taps)
        value_conv = causal_mix(value_up.astype(jnp.float32), feedforward_value_taps)
        hidden = (jax.nn.gelu(gate_conv) * value_conv).astype(jnp.bfloat16)
        branch_ffn = split_partials(hidden, feedforward_down_weight, N_TP).astype(jnp.bfloat16)
        final_rows = middle.astype(jnp.float32) + branch_ffn.astype(jnp.float32)
        inverse = lax.rsqrt(lax.optimization_barrier(jnp.mean(final_rows * final_rows, axis=-1, keepdims=True)) + EPS)
        return (final_rows * inverse * closing_norm_gain).astype(jnp.bfloat16)
    output_rows = lax.map(single_sequence, (stream.reshape(sequence_count, SEQUENCE_TOKENS, MODEL_WIDTH), spike_log_decay.reshape(sequence_count, SEQUENCE_TOKENS, GATE_BLOCKS)))
    return output_rows.reshape(sequence_count * SEQUENCE_TOKENS, MODEL_WIDTH)
```

```python
import functools

import jax
import jax.numpy as jnp
from jax import lax
from jax.experimental import pallas as pl
from jax.experimental.pallas import tpu as pltpu
from jax.sharding import PartitionSpec as P

EPS = 1e-06
GATE_POWER = 8.0


def rms_scale(row_block, gain_vec):
    widened = row_block.astype(jnp.float32)
    inverse = lax.rsqrt(jnp.mean(widened * widened, axis=-1, keepdims=True) + EPS)
    return (widened * inverse * gain_vec).astype(jnp.bfloat16)


def causal_mix(values, kernel_taps):
    extent = kernel_taps.shape[0]
    length = values.shape[0]
    padded = jnp.pad(values, ((extent - 1, 0), (0, 0)))
    summed = kernel_taps[0] * padded[0:length]
    for offset in range(1, extent):
        summed = summed + kernel_taps[offset] * padded[offset : offset + length]
    return summed


def chain_step(earlier, following):
    return (earlier[0] * following[0], following[0] * earlier[1] + following[1])


def fold_pair(source, pieces):
    return (
        jnp.dot(source, pieces[0], preferred_element_type=jnp.float32),
        jnp.dot(source, pieces[1], preferred_element_type=jnp.float32),
    )


def project_with(left_rows, weight_piece):
    return jnp.dot(left_rows, weight_piece, preferred_element_type=jnp.float32).astype(jnp.bfloat16)


def third_rows(rows):
    return rows // 3 // 16 * 16


class RingGather:
    def __init__(self, n, sources, targets, send_sems, recv_sems):
        self.n = n
        self.sources = sources
        self.targets = targets
        self.send_sems = send_sems
        self.recv_sems = recv_sems
        self.rep = lax.axis_index("rep")
        fs = lax.axis_index("fs")
        self.fs = fs
        side = lax.rem(fs, 2)
        depth = fs // 2
        self.place = depth + side * (n - 1 - 2 * depth)

    def member(self, shift):
        place = lax.rem(self.place + shift + 2 * self.n, self.n)
        side = place // (self.n // 2)
        depth = place + side * (self.n - 1 - 2 * place)
        return 2 * depth + side

    def neighbours(self):
        return (
            {"fs": self.member(1)},
            {"fs": self.member(-1)},
            {"rep": 1 - self.rep},
            {"tp": 1 - lax.axis_index("tp")},
        )

    def enter(self):
        barrier = pltpu.get_barrier_semaphore()
        for device in self.neighbours():
            pl.semaphore_signal(
                barrier, inc=1, device_id=device, device_id_type=pl.DeviceIdType.MESH
            )
        pl.semaphore_wait(barrier, 4)

    def piece(self, ref, w, lane, base, other=False):
        rows = self.sources[w].shape[0]
        part = third_rows(rows)
        if lane == 1:
            return ref.at[pl.ds(pl.multiple_of(base + part, 16), rows - 2 * part), :]
        rep = 1 - self.rep if other else self.rep
        return ref.at[pl.ds(pl.multiple_of(base + rep * (rows - part), 16), part), :]

    def heading(self, w, lane):
        return 1 if (w + lane) % 2 == 0 else -1

    def copy(self, w, lane, step, source, target, device):
        return pltpu.make_async_remote_copy(
            src_ref=source,
            dst_ref=target,
            send_sem=self.send_sems.at[w, lane, step],
            recv_sem=self.recv_sems.at[w, lane, step],
            device_id=device,
            device_id_type=pl.DeviceIdType.MESH,
        )

    def hop(self, w, lane, step):
        way = self.heading(w, lane)
        base = self.member(-way * step) * self.sources[w].shape[0]
        target = self.piece(self.targets[w], w, lane, base)
        source = self.piece(self.sources[w], w, lane, 0) if step == 0 else target
        return self.copy(w, lane, step, source, target, {"fs": self.member(way)})

    def arrival(self, w, lane, step):
        way = self.heading(w, lane)
        base = self.member(-way * (step + 1)) * self.sources[w].shape[0]
        target = self.piece(self.targets[w], w, lane, base)
        return self.copy(w, lane, step, target, target, {"fs": self.member(way)})

    def cross(self, w, step, other=False):
        way = self.heading(w, 0)
        if other:
            way_base = self.member(-way * (step + 1)) * self.sources[w].shape[0]
            target = self.piece(self.targets[w], w, 0, way_base, other=True)
        else:
            way_base = self.member(-way * (step + 1)) * self.sources[w].shape[0]
            target = self.piece(self.targets[w], w, 0, way_base)
        return self.copy(w, 2, step, target, target, {"rep": 1 - self.rep})

    def local(self, w, sem):
        rows = self.sources[w].shape[0]
        own = self.targets[w].at[pl.ds(pl.multiple_of(self.fs * rows, 16), rows), :]
        return pltpu.make_async_copy(self.sources[w], own, sem.at[w])

    def start(self, w):
        for lane in (0, 1):
            self.hop(w, lane, 0).start()

    def serve(self, w, step):
        for lane in (0, 1):
            self.arrival(w, lane, step).wait_recv()
            if step + 1 < self.n - 1:
                self.hop(w, lane, step + 1).start()
            if lane == 0:
                self.cross(w, step).start()

    def crossed(self, w):
        for step in range(self.n - 1):
            self.cross(w, step, other=True).wait_recv()

    def drain(self, w):
        for step in range(self.n - 1):
            self.hop(w, 0, step).wait_send()
            self.hop(w, 1, step).wait_send()
            self.cross(w, step).wait_send()


def gather_kernel(n, *refs):
    sources, targets = refs[:6], refs[6:12]
    local_sems, send_sems, recv_sems = refs[12:]
    ring = RingGather(n, sources, targets, send_sems, recv_sems)
    ring.enter()
    for w in range(6):
        ring.local(w, local_sems).start()
    groups = ((0, 1, 2), (3, 4, 5))
    for group in groups:
        for w in group:
            ring.start(w)
        for step in range(n - 1):
            for w in group:
                ring.serve(w, step)
    for w in range(6):
        ring.local(w, local_sems).wait()
        ring.crossed(w)
        ring.drain(w)


def gather_weights(n, weights):
    return pl.pallas_call(
        functools.partial(gather_kernel, n),
        out_shape=[jax.ShapeDtypeStruct((n * w.shape[0], w.shape[1]), w.dtype) for w in weights],
        in_specs=[pl.BlockSpec(memory_space=pl.ANY)] * 6,
        out_specs=[pl.BlockSpec(memory_space=pl.ANY)] * 6,
        scratch_shapes=[
            pltpu.SemaphoreType.DMA((6,)),
            pltpu.SemaphoreType.DMA((6, 3, n - 1)),
            pltpu.SemaphoreType.DMA((6, 3, n - 1)),
        ],
        compiler_params=pltpu.CompilerParams(collective_id=0, has_side_effects=True),
    )(*weights)


def shards(
    ringed,
    stream,
    recurrence_input_weight,
    output_gate_weight,
    recurrence_gate_matrix,
    input_gate_matrix,
    channel_decay_rate,
    recurrence_taps,
    spike_log_decay,
    recurrence_output_weight,
    feedforward_gate_upward,
    feedforward_value_upward,
    feedforward_gate_taps,
    feedforward_value_taps,
    feedforward_down_weight,
    recurrence_norm_gain,
    feedforward_norm_gain,
    closing_norm_gain,
):
    tok_rows = stream.shape[0]
    fs_size = lax.axis_size("fs")
    if ringed:
        weights = list(gather_weights(
            fs_size,
            (
                recurrence_input_weight,
                output_gate_weight,
                recurrence_output_weight,
                feedforward_gate_upward,
                feedforward_value_upward,
                feedforward_down_weight,
            ),
        ))
        for w in (2, 5):
            stacked = weights[w].reshape(fs_size, -1, weights[w].shape[1])
            weights[w] = jnp.concatenate([stacked[f] for f in range(fs_size)], axis=1)
    else:
        weights = [
            lax.all_gather(recurrence_input_weight, "fs", axis=0, tiled=True),
            lax.all_gather(output_gate_weight, "fs", axis=0, tiled=True),
            lax.all_gather(recurrence_output_weight, "fs", axis=1, tiled=True),
            lax.all_gather(feedforward_gate_upward, "fs", axis=0, tiled=True),
            lax.all_gather(feedforward_value_upward, "fs", axis=0, tiled=True),
            lax.all_gather(feedforward_down_weight, "fs", axis=1, tiled=True),
        ]
    head_count = recurrence_gate_matrix.shape[0]
    block_size = recurrence_gate_matrix.shape[1]
    whole_rows = lax.all_gather(stream, "tp", axis=1, tiled=True)
    normed = rms_scale(whole_rows, recurrence_norm_gain)
    rec_sum, gate_sum = fold_pair(
        normed,
        (
            weights[0],
            weights[1],
        ),
    )
    rec_in = rec_sum.astype(jnp.bfloat16)
    gate_src = gate_sum.astype(jnp.bfloat16)
    conv_out = causal_mix(rec_in.astype(jnp.float32), recurrence_taps).astype(jnp.bfloat16)
    blocks = conv_out.reshape(tok_rows, head_count, block_size)
    gate_restart = jax.nn.sigmoid(
        jnp.einsum(
            "thi,hij->thj", blocks, recurrence_gate_matrix, preferred_element_type=jnp.float32
        )
    )
    admit_gate = jax.nn.sigmoid(
        jnp.einsum("thi,hij->thj", blocks, input_gate_matrix, preferred_element_type=jnp.float32)
    )
    decay_base = (GATE_POWER * jax.nn.softplus(-channel_decay_rate)).reshape(head_count, block_size)
    decay_logarithm = -gate_restart * decay_base + spike_log_decay[:, :, None]
    decay_rate = jnp.exp(decay_logarithm)
    inflow = jnp.sqrt(-jnp.expm1(2.0 * decay_logarithm)) * admit_gate * blocks.astype(jnp.float32)
    states = lax.associative_scan(chain_step, (decay_rate, inflow), axis=0)[1]
    mixed_out = (
        states.reshape(tok_rows, head_count * block_size)
        * jax.nn.gelu(gate_src.astype(jnp.float32))
    ).astype(jnp.bfloat16)
    mix_terms = project_with(
        mixed_out, weights[2]
    )
    branch = lax.psum_scatter(
        lax.optimization_barrier(mix_terms).astype(jnp.float32).astype(jnp.bfloat16),
        "tp",
        scatter_dimension=1,
        tiled=True,
    )
    middle = (stream.astype(jnp.float32) + branch.astype(jnp.float32)).astype(jnp.bfloat16)
    whole_middle = lax.all_gather(middle, "tp", axis=1, tiled=True)
    normed_ffn = rms_scale(whole_middle, feedforward_norm_gain)
    gate_sum_ffn, value_sum_ffn = fold_pair(
        normed_ffn,
        (
            weights[3],
            weights[4],
        ),
    )
    gate_up = gate_sum_ffn.astype(jnp.bfloat16)
    value_up = value_sum_ffn.astype(jnp.bfloat16)
    gate_conv = causal_mix(gate_up.astype(jnp.float32), feedforward_gate_taps)
    value_conv = causal_mix(value_up.astype(jnp.float32), feedforward_value_taps)
    hidden = (jax.nn.gelu(gate_conv) * value_conv).astype(jnp.bfloat16)
    down_terms = project_with(
        hidden, weights[5]
    )
    branch_ffn = lax.psum_scatter(
        lax.optimization_barrier(down_terms).astype(jnp.float32).astype(jnp.bfloat16),
        "tp",
        scatter_dimension=1,
        tiled=True,
    )
    final_rows = middle.astype(jnp.float32) + branch_ffn.astype(jnp.float32)
    col_count = final_rows.shape[1]
    square_sum = lax.psum(jnp.sum(final_rows * final_rows, axis=1), "tp")
    inverse = lax.rsqrt(square_sum / (col_count * lax.axis_size("tp")) + EPS)
    gain_part = lax.dynamic_slice_in_dim(
        closing_norm_gain, lax.axis_index("tp") * col_count, col_count
    )
    return (final_rows * inverse[:, None] * gain_part[None, :]).astype(jnp.bfloat16)


def solution(mesh):
    in_specs = (
        P(("rep", "fs"), "tp"),
        P("fs", "tp"),
        P("fs", "tp"),
        P("tp", None, None),
        P("tp", None, None),
        P("tp"),
        P(None, "tp"),
        P(("rep", "fs"), "tp"),
        P("tp", "fs"),
        P("fs", "tp"),
        P("fs", "tp"),
        P(None, "tp"),
        P(None, "tp"),
        P("tp", "fs"),
        P(),
        P(),
        P(),
    )
    out_specs = P(("rep", "fs"), "tp")
    ringed = mesh.shape["rep"] == 2 and mesh.shape["tp"] == 2 and mesh.shape["fs"] == 8
    body = functools.partial(shards, ringed)
    return jax.shard_map(body, mesh=mesh, in_specs=in_specs, out_specs=out_specs, check_vma=False)
```

```python
import functools

import jax
import jax.numpy as jnp
from jax import lax
from jax.experimental import pallas as pl
from jax.experimental.pallas import tpu as pltpu
from jax.sharding import PartitionSpec as P

EPS = 1e-06
GATE_POWER = 8.0


def rms_scale(row_block, gain_vec):
    widened = row_block.astype(jnp.float32)
    inverse = lax.rsqrt(jnp.mean(widened * widened, axis=-1, keepdims=True) + EPS)
    return (widened * inverse * gain_vec).astype(jnp.bfloat16)


def causal_mix(values, kernel_taps):
    extent = kernel_taps.shape[0]
    length = values.shape[0]
    padded = jnp.pad(values, ((extent - 1, 0), (0, 0)))
    summed = kernel_taps[0] * padded[0:length]
    for offset in range(1, extent):
        summed = summed + kernel_taps[offset] * padded[offset : offset + length]
    return summed


def chain_step(earlier, following):
    return (earlier[0] * following[0], following[0] * earlier[1] + following[1])


def fold_pair(source, pieces):
    return (
        jnp.dot(source, pieces[0], preferred_element_type=jnp.float32),
        jnp.dot(source, pieces[1], preferred_element_type=jnp.float32),
    )


def project_with(left_rows, weight_piece):
    return jnp.dot(left_rows, weight_piece, preferred_element_type=jnp.float32).astype(jnp.bfloat16)


def third_rows(rows):
    return rows // 3 // 16 * 16


class RingGather:
    def __init__(self, n, sources, targets, send_sems, recv_sems):
        self.n = n
        self.sources = sources
        self.targets = targets
        self.send_sems = send_sems
        self.recv_sems = recv_sems
        self.rep = lax.axis_index("rep")
        fs = lax.axis_index("fs")
        self.fs = fs
        side = lax.rem(fs, 2)
        depth = fs // 2
        self.place = depth + side * (n - 1 - 2 * depth)

    def member(self, shift):
        place = lax.rem(self.place + shift + 2 * self.n, self.n)
        side = place // (self.n // 2)
        depth = place + side * (self.n - 1 - 2 * place)
        return 2 * depth + side

    def neighbours(self):
        return (
            {"fs": self.member(1)},
            {"fs": self.member(-1)},
            {"rep": 1 - self.rep},
            {"tp": 1 - lax.axis_index("tp")},
        )

    def enter(self):
        barrier = pltpu.get_barrier_semaphore()
        for device in self.neighbours():
            pl.semaphore_signal(
                barrier, inc=1, device_id=device, device_id_type=pl.DeviceIdType.MESH
            )
        pl.semaphore_wait(barrier, 4)

    def piece(self, ref, w, lane, base, other=False):
        rows = self.sources[w].shape[0]
        part = third_rows(rows)
        if lane == 1:
            return ref.at[pl.ds(pl.multiple_of(base + part, 16), rows - 2 * part), :]
        rep = 1 - self.rep if other else self.rep
        return ref.at[pl.ds(pl.multiple_of(base + rep * (rows - part), 16), part), :]

    def heading(self, w, lane):
        return 1 if (w + lane) % 2 == 0 else -1

    def copy(self, w, lane, step, source, target, device):
        return pltpu.make_async_remote_copy(
            src_ref=source,
            dst_ref=target,
            send_sem=self.send_sems.at[w, lane, step],
            recv_sem=self.recv_sems.at[w, lane, step],
            device_id=device,
            device_id_type=pl.DeviceIdType.MESH,
        )

    def hop(self, w, lane, step):
        way = self.heading(w, lane)
        base = self.member(-way * step) * self.sources[w].shape[0]
        target = self.piece(self.targets[w], w, lane, base)
        source = self.piece(self.sources[w], w, lane, 0) if step == 0 else target
        return self.copy(w, lane, step, source, target, {"fs": self.member(way)})

    def arrival(self, w, lane, step):
        way = self.heading(w, lane)
        base = self.member(-way * (step + 1)) * self.sources[w].shape[0]
        target = self.piece(self.targets[w], w, lane, base)
        return self.copy(w, lane, step, target, target, {"fs": self.member(way)})

    def cross(self, w, step, other=False):
        way = self.heading(w, 0)
        if other:
            way_base = self.member(-way * (step + 1)) * self.sources[w].shape[0]
            target = self.piece(self.targets[w], w, 0, way_base, other=True)
        else:
            way_base = self.member(-way * (step + 1)) * self.sources[w].shape[0]
            target = self.piece(self.targets[w], w, 0, way_base)
        return self.copy(w, 2, step, target, target, {"rep": 1 - self.rep})

    def local(self, w, sem):
        rows = self.sources[w].shape[0]
        own = self.targets[w].at[pl.ds(pl.multiple_of(self.fs * rows, 16), rows), :]
        return pltpu.make_async_copy(self.sources[w], own, sem.at[w])

    def start(self, w):
        for lane in (0, 1):
            self.hop(w, lane, 0).start()

    def serve(self, w, step):
        for lane in (0, 1):
            self.arrival(w, lane, step).wait_recv()
            if step + 1 < self.n - 1:
                self.hop(w, lane, step + 1).start()
            if lane == 0:
                self.cross(w, step).start()

    def crossed(self, w):
        for step in range(self.n - 1):
            self.cross(w, step, other=True).wait_recv()

    def drain(self, w):
        for step in range(self.n - 1):
            self.hop(w, 0, step).wait_send()
            self.hop(w, 1, step).wait_send()
            self.cross(w, step).wait_send()


def gelu_of(x):
    return 0.5 * x * (1.0 + jnp.tanh(0.7978845608028654 * (x + 0.044715 * (x * x * x))))


def one_less_exp(z):
    series = 1.0 + z * (1.0 / 6.0)
    for order in (5.0, 4.0, 3.0, 2.0):
        series = 1.0 + z * (1.0 / order) * series
    return jnp.where(z > -0.35, -z * series, 1.0 - jnp.exp(z))


def tap_rows(values, taps_ref, cols):
    extent = taps_ref.shape[0]
    summed = taps_ref[extent - 1 : extent, cols] * values
    row = lax.broadcasted_iota(jnp.int32, values.shape, 0)
    for back in range(1, extent):
        moved = jnp.where(row >= back, pltpu.roll(values, back, 0), 0.0)
        summed = summed + taps_ref[extent - 1 - back : extent - back, cols] * moved
    return summed


def dot32(a, b):
    return jnp.dot(a, b, preferred_element_type=jnp.float32)


def layer_kernel(n, *refs):
    sources = refs[:6]
    (stream, reset_map, admit_map, decay_base, taps, spike) = refs[6:12]
    (gate_taps, value_taps, rec_gain, ffn_gain, last_gain, out) = refs[12:18]
    targets = refs[18:24]
    (stream_in, normed, gate_src, decay, inflow, mixed) = refs[24:30]
    (away, landed, kept, middle, middle_in, hidden, final, sums, sums_in) = refs[30:39]
    local_sems, send_sems, recv_sems, pair_send, pair_recv = refs[39:]
    tokens, width = stream.shape
    me = lax.axis_index("tp")
    ring = RingGather(n, sources, targets, send_sems, recv_sems)
    bf16, f32 = jnp.bfloat16, jnp.float32
    tile = 256
    strip = 48

    def pair(i, source, target):
        return pltpu.make_async_remote_copy(
            src_ref=source,
            dst_ref=target,
            send_sem=pair_send.at[i],
            recv_sem=pair_recv.at[i],
            device_id={"tp": 1 - me},
            device_id_type=pl.DeviceIdType.MESH,
        )

    def half(which):
        return pl.ds(pl.multiple_of(which * width, 128), width)

    def strips(body):
        def step(i, carry):
            body(pl.ds(pl.multiple_of(i * strip, 16), strip))
            return carry

        lax.fori_loop(0, tokens // strip, step, 0)

    def norm_into(mine, theirs, gain):
        def body(rows):
            a = mine[rows, :].astype(f32)
            b = theirs[rows, :].astype(f32)
            total = jnp.sum(a * a, axis=1, keepdims=True) + jnp.sum(b * b, axis=1, keepdims=True)
            inverse = lax.rsqrt(total * (1.0 / (2 * width)) + EPS)
            normed[rows, half(me)] = (a * inverse * gain[:, half(me)]).astype(bf16)
            normed[rows, half(1 - me)] = (b * inverse * gain[:, half(1 - me)]).astype(bf16)

        strips(body)

    def project(i, rows, w):
        depth = rows.shape[1]
        per_half = n // 2

        def into(target, which):
            def step(j, carry):
                slot = which * per_half + j
                block = targets[w][pl.ds(pl.multiple_of(slot * depth, 16), depth), :]
                cols = pl.ds(pl.multiple_of(j * tile, 128), tile)
                target[:, cols] = dot32(rows[...], block).astype(bf16)
                return carry

            lax.fori_loop(0, per_half, step, 0)

        into(away.at[i], 1 - me)
        sent = pair(1 + i, away.at[i], landed.at[i])
        sent.start()
        into(kept, me)
        sent.wait()

    def ready(w):
        ring.local(w, local_sems).wait()
        ring.crossed(w)

    ring.enter()
    first = pair(0, stream, stream_in)
    first.start()
    for w in range(3):
        ring.start(w)
    for w in range(6):
        ring.local(w, local_sems).start()
    first.wait()
    norm_into(stream, stream_in, rec_gain)
    for step in range(n - 1):
        for w in range(3):
            ring.serve(w, step)
        if step == n - 3:
            ring.start(3)
            ring.start(4)
    for w in range(3):
        ready(w)

    def ticks(step):
        ring.serve(3, step)
        ring.serve(4, step)

    for c in range(width // tile):
        cols = slice(c * tile, (c + 1) * tile)
        rec = dot32(normed[...], targets[0][:, cols]).astype(bf16).astype(f32)
        conv = tap_rows(rec, taps, cols).astype(bf16)
        gate_src[:, cols] = dot32(normed[...], targets[1][:, cols]).astype(bf16)
        for part in range(tile // 128):
            h = c * (tile // 128) + part
            lanes = slice(h * 128, (h + 1) * 128)
            block = conv[:, part * 128 : (part + 1) * 128]
            reset = jax.nn.sigmoid(dot32(block, reset_map[h]))
            admit = jax.nn.sigmoid(dot32(block, admit_map[h]))
            log_decay = spike[:, h : h + 1] - reset * decay_base[:, lanes]
            decay[:, lanes] = jnp.exp(log_decay)
            inflow[:, lanes] = jnp.sqrt(one_less_exp(2.0 * log_decay)) * admit * block.astype(f32)
        ticks(c)

    row = lax.broadcasted_iota(jnp.int32, (8, width), 0)

    def scan_step(i, carry):
        rows = pl.ds(pl.multiple_of(i * 16, 16), 16)
        a16, b16 = decay[rows, :], inflow[rows, :]
        found = []
        for part in range(2):
            a, b = a16[part * 8 : part * 8 + 8], b16[part * 8 : part * 8 + 8]
            for back in (1, 2, 4):
                a_before = jnp.where(row >= back, pltpu.roll(a, back, 0), 1.0)
                b_before = jnp.where(row >= back, pltpu.roll(b, back, 0), 0.0)
                b = a * b_before + b
                a = a * a_before
            states = a * carry + b
            carry = states[7:8, :]
            found.append(states)
        states = jnp.concatenate(found, axis=0)
        mixed[rows, :] = (states * gelu_of(gate_src[rows, :].astype(f32))).astype(bf16)
        return carry

    lax.fori_loop(0, tokens // 16, scan_step, jnp.zeros((1, width), f32))
    served = width // tile
    ticks(served)
    project(0, mixed, 2)

    def add_branch(rows):
        branch = (kept[rows, :].astype(f32) + landed[0, rows, :].astype(f32)).astype(bf16)
        middle[rows, :] = (stream[rows, :].astype(f32) + branch.astype(f32)).astype(bf16)

    strips(add_branch)
    shared = pair(3, middle, middle_in)
    shared.start()
    ring.start(5)
    shared.wait()
    for step in range(served + 1, n - 1):
        ticks(step)
        if step == served + 1:
            norm_into(middle, middle_in, ffn_gain)
    ready(3)
    ready(4)

    def up_step(t, carry):
        cols = pl.ds(pl.multiple_of(t * tile, 128), tile)
        gate = dot32(normed[...], targets[3][:, cols]).astype(bf16).astype(f32)
        gate = gelu_of(tap_rows(gate, gate_taps, cols))
        value = dot32(normed[...], targets[4][:, cols]).astype(bf16).astype(f32)
        hidden[:, cols] = (gate * tap_rows(value, value_taps, cols)).astype(bf16)
        return carry

    tiles = hidden.shape[1] // tile
    for step in range(n - 1):
        lax.fori_loop(step * tiles // (n - 1), (step + 1) * tiles // (n - 1), up_step, 0)
        ring.serve(5, step)
    ready(5)
    project(1, hidden, 5)

    def finish(rows):
        branch = (kept[rows, :].astype(f32) + landed[1, rows, :].astype(f32)).astype(bf16)
        total = middle[rows, :].astype(f32) + branch.astype(f32)
        final[rows, :] = total
        square = jnp.sum(total * total, axis=1, keepdims=True)
        sums[rows, :] = jnp.broadcast_to(square, (strip, 128))

    strips(finish)
    summed = pair(4, sums, sums_in)
    summed.start()
    summed.wait()

    def scale(rows):
        square = sums[rows, :] + sums_in[rows, :]
        inverse = lax.rsqrt(square * (1.0 / (2 * width)) + EPS)[:, 0:1]
        out[rows, :] = (final[rows, :] * inverse * last_gain[:, half(me)]).astype(bf16)

    strips(scale)
    for w in range(6):
        ring.drain(w)


def fused_layer(n, weights, others):
    tokens, width = others[0].shape
    wide = weights[3].shape[1]
    bf16, f32 = jnp.bfloat16, jnp.float32
    vmem = pltpu.VMEM
    return pl.pallas_call(
        functools.partial(layer_kernel, n),
        out_shape=jax.ShapeDtypeStruct((tokens, width), bf16),
        in_specs=[pl.BlockSpec(memory_space=pl.ANY)] * 6
        + [pl.BlockSpec(memory_space=vmem)] * len(others),
        out_specs=pl.BlockSpec(memory_space=vmem),
        scratch_shapes=[vmem((n * w.shape[0], w.shape[1]), w.dtype) for w in weights]
        + [
            vmem((tokens, width), bf16),
            vmem((tokens, 2 * width), bf16),
            vmem((tokens, width), bf16),
            vmem((tokens, width), f32),
            vmem((tokens, width), f32),
            vmem((tokens, width), bf16),
            vmem((2, tokens, width), bf16),
            vmem((2, tokens, width), bf16),
            vmem((tokens, width), bf16),
            vmem((tokens, width), bf16),
            vmem((tokens, width), bf16),
            vmem((tokens, wide), bf16),
            vmem((tokens, width), f32),
            vmem((tokens, 128), f32),
            vmem((tokens, 128), f32),
            pltpu.SemaphoreType.DMA((6,)),
            pltpu.SemaphoreType.DMA((6, 3, n - 1)),
            pltpu.SemaphoreType.DMA((6, 3, n - 1)),
            pltpu.SemaphoreType.DMA((5,)),
            pltpu.SemaphoreType.DMA((5,)),
        ],
        compiler_params=pltpu.CompilerParams(
            collective_id=0, has_side_effects=True, vmem_limit_bytes=66_000_000
        ),
    )(*weights, *others)


def shards(
    ringed,
    stream,
    recurrence_input_weight,
    output_gate_weight,
    recurrence_gate_matrix,
    input_gate_matrix,
    channel_decay_rate,
    recurrence_taps,
    spike_log_decay,
    recurrence_output_weight,
    feedforward_gate_upward,
    feedforward_value_upward,
    feedforward_gate_taps,
    feedforward_value_taps,
    feedforward_down_weight,
    recurrence_norm_gain,
    feedforward_norm_gain,
    closing_norm_gain,
):
    tok_rows = stream.shape[0]
    fs_size = lax.axis_size("fs")
    if ringed:
        return fused_layer(
            fs_size,
            (
                recurrence_input_weight,
                output_gate_weight,
                recurrence_output_weight,
                feedforward_gate_upward,
                feedforward_value_upward,
                feedforward_down_weight,
            ),
            (
                stream,
                recurrence_gate_matrix,
                input_gate_matrix,
                (GATE_POWER * jax.nn.softplus(-channel_decay_rate))[None, :],
                recurrence_taps,
                spike_log_decay,
                feedforward_gate_taps,
                feedforward_value_taps,
                recurrence_norm_gain[None, :],
                feedforward_norm_gain[None, :],
                closing_norm_gain[None, :],
            ),
        )
    weights = [
        lax.all_gather(recurrence_input_weight, "fs", axis=0, tiled=True),
        lax.all_gather(output_gate_weight, "fs", axis=0, tiled=True),
        lax.all_gather(recurrence_output_weight, "fs", axis=1, tiled=True),
        lax.all_gather(feedforward_gate_upward, "fs", axis=0, tiled=True),
        lax.all_gather(feedforward_value_upward, "fs", axis=0, tiled=True),
        lax.all_gather(feedforward_down_weight, "fs", axis=1, tiled=True),
    ]
    head_count = recurrence_gate_matrix.shape[0]
    block_size = recurrence_gate_matrix.shape[1]
    whole_rows = lax.all_gather(stream, "tp", axis=1, tiled=True)
    normed = rms_scale(whole_rows, recurrence_norm_gain)
    rec_sum, gate_sum = fold_pair(
        normed,
        (
            weights[0],
            weights[1],
        ),
    )
    rec_in = rec_sum.astype(jnp.bfloat16)
    gate_src = gate_sum.astype(jnp.bfloat16)
    conv_out = causal_mix(rec_in.astype(jnp.float32), recurrence_taps).astype(jnp.bfloat16)
    blocks = conv_out.reshape(tok_rows, head_count, block_size)
    gate_restart = jax.nn.sigmoid(
        jnp.einsum(
            "thi,hij->thj", blocks, recurrence_gate_matrix, preferred_element_type=jnp.float32
        )
    )
    admit_gate = jax.nn.sigmoid(
        jnp.einsum("thi,hij->thj", blocks, input_gate_matrix, preferred_element_type=jnp.float32)
    )
    decay_base = (GATE_POWER * jax.nn.softplus(-channel_decay_rate)).reshape(head_count, block_size)
    decay_logarithm = -gate_restart * decay_base + spike_log_decay[:, :, None]
    decay_rate = jnp.exp(decay_logarithm)
    inflow = jnp.sqrt(-jnp.expm1(2.0 * decay_logarithm)) * admit_gate * blocks.astype(jnp.float32)
    states = lax.associative_scan(chain_step, (decay_rate, inflow), axis=0)[1]
    mixed_out = (
        states.reshape(tok_rows, head_count * block_size)
        * jax.nn.gelu(gate_src.astype(jnp.float32))
    ).astype(jnp.bfloat16)
    mix_terms = project_with(
        mixed_out, weights[2]
    )
    branch = lax.psum_scatter(
        lax.optimization_barrier(mix_terms).astype(jnp.float32).astype(jnp.bfloat16),
        "tp",
        scatter_dimension=1,
        tiled=True,
    )
    middle = (stream.astype(jnp.float32) + branch.astype(jnp.float32)).astype(jnp.bfloat16)
    whole_middle = lax.all_gather(middle, "tp", axis=1, tiled=True)
    normed_ffn = rms_scale(whole_middle, feedforward_norm_gain)
    gate_sum_ffn, value_sum_ffn = fold_pair(
        normed_ffn,
        (
            weights[3],
            weights[4],
        ),
    )
    gate_up = gate_sum_ffn.astype(jnp.bfloat16)
    value_up = value_sum_ffn.astype(jnp.bfloat16)
    gate_conv = causal_mix(gate_up.astype(jnp.float32), feedforward_gate_taps)
    value_conv = causal_mix(value_up.astype(jnp.float32), feedforward_value_taps)
    hidden = (jax.nn.gelu(gate_conv) * value_conv).astype(jnp.bfloat16)
    down_terms = project_with(
        hidden, weights[5]
    )
    branch_ffn = lax.psum_scatter(
        lax.optimization_barrier(down_terms).astype(jnp.float32).astype(jnp.bfloat16),
        "tp",
        scatter_dimension=1,
        tiled=True,
    )
    final_rows = middle.astype(jnp.float32) + branch_ffn.astype(jnp.float32)
    col_count = final_rows.shape[1]
    square_sum = lax.psum(jnp.sum(final_rows * final_rows, axis=1), "tp")
    inverse = lax.rsqrt(square_sum / (col_count * lax.axis_size("tp")) + EPS)
    gain_part = lax.dynamic_slice_in_dim(
        closing_norm_gain, lax.axis_index("tp") * col_count, col_count
    )
    return (final_rows * inverse[:, None] * gain_part[None, :]).astype(jnp.bfloat16)


def solution(mesh):
    in_specs = (
        P(("rep", "fs"), "tp"),
        P("fs", "tp"),
        P("fs", "tp"),
        P("tp", None, None),
        P("tp", None, None),
        P("tp"),
        P(None, "tp"),
        P(("rep", "fs"), "tp"),
        P("tp", "fs"),
        P("fs", "tp"),
        P("fs", "tp"),
        P(None, "tp"),
        P(None, "tp"),
        P("tp", "fs"),
        P(),
        P(),
        P(),
    )
    out_specs = P(("rep", "fs"), "tp")
    ringed = mesh.shape["rep"] == 2 and mesh.shape["tp"] == 2 and mesh.shape["fs"] == 8
    body = functools.partial(shards, ringed)
    return jax.shard_map(body, mesh=mesh, in_specs=in_specs, out_specs=out_specs, check_vma=False)
```
